32 devices in a mesh: grp: 2 (over x), sp: 4 (over z), tp: 4 (over y, core).
Axes of the slice: x: 2, y: 2, z: 4, core: 2. Of those that a mesh axis runs over, the one named last changes fastest.
Arguments:
- tokens: bfloat16 [4, 1024, 2048], P('grp', 'sp'), parts along dimension 0, may hold values from -6 to 6
- decoded_input: bfloat16 [4, 2048], P('grp'), parts along dimension 0, may hold values from -6 to 6
- query_weight: bfloat16 [2048, 4096], P(None, 'tp'), may hold values from -0.125 to 0.125
- key_weight: bfloat16 [2048, 4096], P(None, 'tp'), may hold values from -0.125 to 0.125
- value_weight: bfloat16 [2048, 4096], P(None, 'tp'), may hold values from -0.125 to 0.125
- gate_weight: bfloat16 [2048, 2, 32], replicated, may hold values from -0.125 to 0.125
- head_decay_rate: float32 [32], P('tp'), may hold values from 9.765625e-05 to 0.08, as said below
- extra_log_decay: float32 [4, 32, 1024], P('grp', 'tp', 'sp'), parts along dimension 0, may hold values from -2.8 to 0, as said below
- read_norm_gain: float32 [128], replicated, may hold values from 0.1 to 1.9
Outputs:
- cache: bfloat16 [4, 32, 128, 128], P('grp', 'tp', 'sp'), parts along dimension 0
- read: bfloat16 [4, 4096], P('grp', 'tp'), parts along dimension 0
The draws below stay inside these ranges and needn't reach their ends.
There are 2 independent parts, one for each index of `grp`. The reference program is written for one: setup_inputs(seed, part) draws one part's arguments, and reference() takes and returns one part's arrays. A program takes and returns all parts, laid end to end along the dimension named above; an argument that names none is the same for every part. Nothing has to cross between parts.
Inputs may be any that keep to these rules, and one draw needn't show every extreme that they name: `head_decay_rate`: positive. `extra_log_decay`: zero at all but a few positions.
All inputs are finite; a program needn't handle non-finite values.
Results may differ from the reference program's by a relative error of at most 0.002.
Values sent between devices are 32-bit elements; how exact they have to be, the bound alone decides.
A program may use at most 64 MiB of HBM per device.

```python
import jax
import jax.numpy as jnp
from jax import lax

D = 2048
H = 32
HEAD = 128
BLOCK = 64
SEQS = 2
LEN = 1024


def draw_head_decay_rate(key, part):
    span = 1.0 * LEN
    slow = jnp.exp(jax.random.uniform(jax.random.fold_in(key, 21), (H,), jnp.float32, jnp.log(0.1 / span), jnp.log(1.5 / span)))
    fast = jax.random.uniform(jax.random.fold_in(key, 22), (H,), jnp.float32, 0.02, 0.08)
    picked = jax.random.bernoulli(jax.random.fold_in(key, 23), 0.5, (H,))
    return jnp.where(picked, fast, slow).astype(jnp.float32)


def draw_extra_log_decay(key, part):
    places = jax.random.randint(jax.random.fold_in(key, 11), (SEQS, H, 4), 0, LEN)
    depths = jax.random.uniform(jax.random.fold_in(key, 12), (SEQS, H, 4), jnp.float32, jnp.log(0.5), jnp.log(0.8))
    where = jnp.arange(LEN)
    marks = jnp.where(where[None, None, None, :] == places[..., None], depths[..., None], 0.0)
    return jnp.sum(marks, axis=2).astype(jnp.float32)


def block_levels(own_key, shape, shards, low, high):
    level = 1.0
    for dim, parts in shards:
        heights = jax.random.uniform(jax.random.fold_in(jax.random.fold_in(own_key, 6), dim), (parts,), jnp.float32, low / len(shards), high / len(shards))
        level = level * jnp.repeat(jnp.exp(heights), shape[dim] // parts).reshape((-1,) + (1,) * (len(shape) - 1 - dim))
    return level


def scatter_about(stream_key, dims, scale, reach, pieces=(), kind=jnp.bfloat16):
    entries = jax.random.normal(stream_key, dims, jnp.float32) * scale
    if len(pieces) > 0:
        entries = block_levels(stream_key, dims, pieces, -0.22, 0.18) * entries
    return jnp.clip(entries, min=-reach, max=reach).astype(kind)


def setup_inputs(seed: int = 0, part: int = 0) -> dict:
    streams_of = jax.random.split(jax.random.key(seed), 10)
    own_keys = jax.random.split(jax.random.fold_in(streams_of[9], part), 10)
    tokens = scatter_about(own_keys[0], (SEQS, LEN, D), 1.0, 6.0, ((1, 4),))
    decoded_input = scatter_about(own_keys[1], (SEQS, D), 1.0, 6.0)
    query_weight = scatter_about(streams_of[2], (D, H * HEAD), D ** -0.5, 0.125, ((1, 4),))
    key_weight = scatter_about(streams_of[3], (D, H * HEAD), D ** -0.5, 0.125, ((1, 4),))
    value_weight = scatter_about(streams_of[4], (D, H * HEAD), D ** -0.5, 0.125, ((1, 4),))
    gate_weight = scatter_about(streams_of[5], (D, 2, H), D ** -0.5, 0.125)
    head_decay_rate = draw_head_decay_rate(jax.random.fold_in(streams_of[9], 71), part)
    extra_log_decay = draw_extra_log_decay(jax.random.fold_in(jax.random.fold_in(streams_of[9], part), 71), part)
    read_norm_gain = jnp.clip(1.0 + 0.18 * jax.random.normal(streams_of[8], (HEAD,), jnp.float32), 0.1, 1.9)
    return dict(tokens=tokens, decoded_input=decoded_input, query_weight=query_weight, key_weight=key_weight, value_weight=value_weight, gate_weight=gate_weight, head_decay_rate=head_decay_rate, extra_log_decay=extra_log_decay, read_norm_gain=read_norm_gain)


epsilon = 1e-06
write_offset = 5.0
highest = lax.Precision.HIGHEST

def unit_rows(vectors):
    return vectors * lax.rsqrt(lax.optimization_barrier(jnp.sum(vectors * vectors, axis=-1, keepdims=True)) + epsilon)

def project(flat, key_weight, value_weight, gate_cols, head_decay_rate, head_total, head_dim):
    keys = jax.nn.silu(jnp.dot(flat.astype(jnp.float32), key_weight.astype(jnp.float32), preferred_element_type=jnp.float32))
    keys = unit_rows(keys.reshape(flat.shape[0], head_total, head_dim))
    values = jax.nn.silu(jnp.dot(flat.astype(jnp.float32), value_weight.astype(jnp.float32), preferred_element_type=jnp.float32))
    values = values.reshape(flat.shape[0], head_total, head_dim)
    gates = jnp.dot(flat.astype(jnp.float32), gate_cols.astype(jnp.float32), preferred_element_type=jnp.float32)
    beta = jax.nn.sigmoid(gates[:, :head_total] - write_offset)
    decay_factor = -head_decay_rate * jax.nn.softplus(gates[:, head_total:])
    return (keys, values, beta, decay_factor)

def block_parts(keys, values, beta, decay_factor):
    size = keys.shape[-2]
    head_dim = values.shape[-1]
    running = jnp.cumsum(decay_factor, axis=-1)
    index = jnp.arange(size)
    strict = index[:, None] > index[None, :]
    spread = running[..., :, None] - running[..., None, :]
    below = jnp.where(strict, jnp.exp(jnp.where(strict, spread, 0.0)), 0.0)
    inner = jnp.einsum('...id,...jd->...ij', keys, keys, precision=highest)
    lower = jnp.eye(size, dtype=jnp.float32) + beta[..., :, None] * inner * below
    right = jnp.concatenate([values * beta[..., None], keys * (beta * jnp.exp(running))[..., None]], axis=-1)
    solved = jax.scipy.linalg.solve_triangular(lower, right, lower=True, unit_diagonal=True)
    total = jnp.exp(running[..., -1])
    carried = keys * jnp.exp(running[..., -1:] - running)[..., None]
    return (solved[..., :head_dim], solved[..., head_dim:], total, carried)

def reference(tokens, decoded_input, query_weight, key_weight, value_weight, gate_weight, head_decay_rate, extra_log_decay, read_norm_gain):
    sequence_total, prompt_length, width = tokens.shape
    head_total = head_decay_rate.shape[0]
    head_dim = key_weight.shape[1] // head_total
    gate_cols = gate_weight.reshape(width, 2 * head_total)
    flat = tokens.reshape(sequence_total * prompt_length, width)
    keys, values, beta, decay_factor = project(flat, key_weight, value_weight, gate_cols, head_decay_rate, head_total, head_dim)
    count = prompt_length // BLOCK
    keys_b = keys.reshape(sequence_total, count, BLOCK, head_total, head_dim).transpose(1, 0, 3, 2, 4)
    values_b = values.reshape(sequence_total, count, BLOCK, head_total, head_dim).transpose(1, 0, 3, 2, 4)
    beta_b = beta.reshape(sequence_total, count, BLOCK, head_total).transpose(1, 0, 3, 2)
    decay_every_token = decay_factor.reshape(sequence_total, prompt_length, head_total).transpose(0, 2, 1) + extra_log_decay
    decay_b = decay_every_token.reshape(sequence_total, head_total, count, BLOCK).transpose(2, 0, 1, 3)

    def advance(state, block):
        solved_u, solved_w, total, carried = block_parts(block[0], block[1], block[2], block[3])
        delta = solved_u - jnp.einsum('shcd,shdv->shcv', solved_w, state, precision=highest)
        state = total[..., None, None] * state + jnp.einsum('shcd,shcv->shdv', carried, delta, precision=highest)
        return (state, None)
    start = jnp.zeros((sequence_total, head_total, head_dim, head_dim), jnp.float32)
    final, _ = lax.scan(advance, start, (keys_b, values_b, beta_b, decay_b))
    query = jax.nn.silu(jnp.dot(decoded_input.astype(jnp.float32), query_weight.astype(jnp.float32), preferred_element_type=jnp.float32)).reshape(sequence_total, head_total, head_dim)
    new_key, new_value, new_beta, new_decay = project(decoded_input, key_weight, value_weight, gate_cols, head_decay_rate, head_total, head_dim)
    keep = jnp.exp(new_decay)
    key_read = jnp.einsum('shd,shdv->shv', new_key, final, precision=highest)
    query_read = jnp.einsum('shd,shdv->shv', query, final, precision=highest)
    intersection = lax.optimization_barrier(jnp.sum(query * new_key, axis=-1))
    cache = keep[..., None, None] * final - (keep * new_beta)[..., None, None] * new_key[..., :, None] * key_read[..., None, :] + new_beta[..., None, None] * new_key[..., :, None] * new_value[..., None, :]
    mixed = keep[..., None] * query_read - (keep * new_beta * intersection)[..., None] * key_read + (new_beta * intersection)[..., None] * new_value
    normed = mixed * lax.rsqrt(lax.optimization_barrier(jnp.mean(mixed * mixed, axis=-1, keepdims=True)) + epsilon) * read_norm_gain
    return (cache.astype(jnp.bfloat16), normed.reshape(sequence_total, head_total * head_dim).astype(jnp.bfloat16))
```

```python
import functools

import jax
import jax.numpy as jnp
from jax import lax
from jax.experimental import pallas as pl
from jax.experimental.pallas import tpu as pltpu
from jax.sharding import PartitionSpec as P

epsilon = 1e-06
write_offset = 5.0
f32 = jnp.float32
bf16 = jnp.bfloat16
MESH = pl.DeviceIdType.MESH
ROWS = (((1,), (0,)), ((), ()))
SAME = (((1,), (1,)), ((), ()))
OUTER = (((0,), (0,)), ((), ()))


def dot(a, b, dims=ROWS):
    return lax.dot_general(a, b, dims, preferred_element_type=f32)


def split(x):
    high = x.astype(bf16)
    return high, (x - high.astype(f32)).astype(bf16)


def dot3(a, b, dims=ROWS):
    ah, al = a
    bh, bl = b
    return dot(ah, bh, dims) + (dot(ah, bl, dims) + dot(al, bh, dims))


def silu(x):
    return x * jax.nn.sigmoid(x)


def unit_rows(x):
    return x * lax.rsqrt(jnp.sum(x * x, axis=-1, keepdims=True) + epsilon)


def span_solve(lower, right):
    size = lower.shape[0]
    row = lax.broadcasted_iota(jnp.int32, (size, size), 0)
    col = lax.broadcasted_iota(jnp.int32, (size, size), 1)
    eye = jnp.where(row == col, 1.0, 0.0)
    inverse = eye - jnp.where((row % 2 == 1) & (col == row - 1), lower, 0.0)
    width = 2
    while width < size:
        pick = (row // width % 2 == 1) & (col // width == row // width - 1)
        part = jnp.where(pick, lower, 0.0).astype(bf16)
        coarse = inverse.astype(bf16)
        inverse = inverse - dot(coarse, dot(part, coarse).astype(bf16))
        width *= 2
    coarse = inverse.astype(bf16)
    first = dot(coarse, right.astype(bf16))
    residual = (right - first) - dot3(split(lower), split(first))
    return first + dot(coarse, residual.astype(bf16))


def kernel(
    parts,
    tok,
    dec,
    kw,
    vw,
    qw,
    gates_t,
    rate,
    extra,
    gain,
    cache_o,
    read_o,
    x,
    rows_s,
    cols_s,
    decg,
    a_buf,
    b_buf,
    d_buf,
    s_recv,
    s_send,
    fin,
    rfin,
    tok_sem,
    s_send_sem,
    s_recv_sem,
    f_send_sem,
    f_recv_sem,
):
    groups = a_buf.shape[0]
    seqs, span, width = tok.shape
    total_rows = seqs * span
    head_dim = kw.shape[1]
    padded = rate.shape[0]
    share = head_dim // parts
    step = pl.program_id(0)
    me = lax.axis_index("sp")
    last = parts - 1
    barrier = pltpu.get_barrier_semaphore()

    @pl.when(step == 0)
    def _():
        for other in range(parts):

            @pl.when(me != other)
            def _():
                pl.semaphore_signal(
                    barrier, inc=1, device_id={"sp": other}, device_id_type=MESH
                )

        loads = [
            pltpu.make_async_copy(tok.at[s], x.at[pl.ds(s * span, span)], tok_sem.at[s])
            for s in range(seqs)
        ]
        for load in loads:
            load.start()
        x[total_rows:, :] = jnp.zeros((x.shape[0] - total_rows, width), bf16)
        x[total_rows : total_rows + seqs, :] = dec[...]
        for load in loads:
            load.wait()
        gates = dot(gates_t[...], x[...], SAME)
        beta = jax.nn.sigmoid(gates[:padded] - write_offset)
        raw = gates[padded:]
        soft = jnp.maximum(raw, 0.0) + jnp.log1p(jnp.exp(-jnp.abs(raw)))
        decay = -rate[...] * soft
        decg[:padded, :] = beta[:, total_rows:]
        decg[padded:, :] = jnp.exp(decay[:, total_rows:])
        row = lax.broadcasted_iota(jnp.int32, (span, span), 0)
        col = lax.broadcasted_iota(jnp.int32, (span, span), 1)
        upto = jnp.where(row <= col, 1.0, 0.0).astype(bf16)
        for s in range(seqs):
            mine = decay[:, s * span : (s + 1) * span] + extra[s]
            high, rest = split(mine)
            rest_f = mine - high.astype(f32)
            low = (rest_f - rest.astype(f32)).astype(bf16)
            running = dot(high, upto) + (dot(rest, upto) + dot(low, upto))
            rows_s[:padded, s * span : (s + 1) * span] = beta[:, s * span : (s + 1) * span]
            rows_s[padded : 2 * padded, s * span : (s + 1) * span] = running
        rows_s[2 * padded :, :] = jnp.zeros((rows_s.shape[0] - 2 * padded, total_rows), f32)
        cols_s[...] = rows_s[...].T
        pl.semaphore_wait(barrier, parts - 1)

    @pl.when(step < groups)
    def _():
        weights = jnp.concatenate([kw[...], vw[...]], axis=1)
        used = total_rows + 16
        both = silu(dot(x[:used, :], weights))
        keys = unit_rows(both[:, :head_dim])
        values = both[:, head_dim:]
        query = silu(dot(x[total_rows:used, :], qw[...]))
        lane = lax.broadcasted_iota(jnp.int32, (span, cols_s.shape[1]), 1)
        row = lax.broadcasted_iota(jnp.int32, (span, span), 0)
        col = lax.broadcasted_iota(jnp.int32, (span, span), 1)
        strict = row > col
        hrow = lax.broadcasted_iota(jnp.int32, (head_dim, head_dim), 0)
        hcol = lax.broadcasted_iota(jnp.int32, (head_dim, head_dim), 1)
        for s in range(seqs):
            at = total_rows + s
            d_buf[step, s, 0:1, :] = keys[at : at + 1]
            d_buf[step, s, 1:2, :] = query[s : s + 1]
            d_buf[step, s, 2:3, :] = values[at : at + 1]
            k = keys[s * span : (s + 1) * span]
            v = values[s * span : (s + 1) * span]
            table = cols_s[s * span : (s + 1) * span, :]
            beta = jnp.sum(jnp.where(lane == step, table, 0.0), axis=1, keepdims=True)
            run = jnp.sum(
                jnp.where(lane == padded + step, table, 0.0), axis=1, keepdims=True
            )
            run_row = rows_s[pl.ds(padded + step, 1), s * span : (s + 1) * span]
            end = run[span - 1 :, :]
            spread = jnp.where(strict, run - run_row, 0.0)
            below = jnp.where(strict, jnp.exp(spread), 0.0)
            kk = split(k)
            lower = beta * dot3(kk, kk, SAME) * below
            right = jnp.concatenate([v * beta, k * (beta * jnp.exp(run))], axis=1)
            solved = span_solve(lower, right)
            carried = (k * jnp.exp(end - run)).T
            moved = dot3(split(carried), split(solved))
            b_buf[step, s] = moved[:, :head_dim]
            a_buf[step, s] = (
                jnp.where(hrow == hcol, jnp.exp(end), 0.0) - moved[:, head_dim:]
            )

    def state_copy(c, right):
        return pltpu.make_async_remote_copy(
            src_ref=s_send.at[c],
            dst_ref=s_recv.at[c],
            send_sem=s_send_sem.at[c],
            recv_sem=s_recv_sem.at[c],
            device_id={"sp": right},
            device_id_type=MESH,
        )

    def share_copy(c, to):
        return pltpu.make_async_remote_copy(
            src_ref=fin.at[c, to],
            dst_ref=rfin.at[c],
            send_sem=f_send_sem.at[c, to],
            recv_sem=f_recv_sem.at[c],
            device_id={"sp": to},
            device_id_type=MESH,
        )

    group = step - me
    busy = (group >= 0) & (group < groups)
    right_of = jnp.minimum(me + 1, last)

    @pl.when(busy & (me == 0))
    def _():
        s_send[group] = b_buf[group]
        state_copy(group, right_of).start()

    def advance(s):
        return dot3(split(a_buf[group, s]), split(s_recv[group, s])) + b_buf[group, s]

    @pl.when(busy & (me > 0) & (me < last))
    def _():
        state_copy(group, right_of).wait_recv()
        for s in range(seqs):
            s_send[group, s] = advance(s)
        state_copy(group, right_of).start()

    @pl.when(busy & (me == last))
    def _():
        state_copy(group, 0).wait_recv()
        eight = lax.broadcasted_iota(jnp.int32, (8, head_dim), 0)
        for s in range(seqs):
            final = advance(s)
            rows = d_buf[group, s]
            new_key, query, new_value = rows[0:1], rows[1:2], rows[2:3]
            reads = dot3(split(rows), split(final))
            key_read, query_read = reads[0:1], reads[1:2]
            beta = decg[pl.ds(group, 1), s : s + 1]
            keep = decg[pl.ds(padded + group, 1), s : s + 1]
            meet = jnp.sum(query * new_key, axis=-1, keepdims=True)
            delta = beta * new_value - (keep * beta) * key_read
            key_pad = jnp.where(eight == 0, new_key, 0.0)
            delta_pad = jnp.where(eight == 0, delta, 0.0)
            outer = dot3(split(key_pad), split(delta_pad), OUTER)
            state = keep * final + outer
            mixed = (
                keep * query_read
                - (keep * beta * meet) * key_read
                + (beta * meet) * new_value
            )
            normed = (
                mixed
                * lax.rsqrt(jnp.mean(mixed * mixed, axis=-1, keepdims=True) + epsilon)
                * gain[...]
            )
            normed = jnp.broadcast_to(normed, (8, head_dim))
            for to in range(last):
                fin[group, to, s, :share] = state[to * share : (to + 1) * share]
                fin[group, to, s, share:] = normed
            rfin[group, s, :share] = state[last * share :]
            rfin[group, s, share:] = normed
        for to in range(last):
            share_copy(group, to).start()

    @pl.when(step == groups - 1 + last)
    def _():
        @pl.when(me < last)
        def _():
            for c in range(groups):
                state_copy(c, right_of).wait_send()
                share_copy(c, 0).wait_recv()

        @pl.when(me == last)
        def _():
            for c in range(groups):
                for to in range(last):
                    share_copy(c, to).wait_send()

        for c in range(groups):
            for s in range(seqs):
                cache_o[s, c] = rfin[c, s, :share].astype(bf16)
                read_o[s : s + 1, c * head_dim : (c + 1) * head_dim] = rfin[
                    c, s, share : share + 1
                ].astype(bf16)


def per_device(
    parts,
    tokens,
    decoded_input,
    query_weight,
    key_weight,
    value_weight,
    gate_weight,
    head_decay_rate,
    extra_log_decay,
    read_norm_gain,
):
    seqs, span, width = tokens.shape
    heads = head_decay_rate.shape[0]
    head_dim = key_weight.shape[1] // heads
    share = head_dim // parts
    padded = -(-heads // 8) * 8
    first = lax.axis_index("tp") * heads
    gates = lax.dynamic_slice_in_dim(gate_weight, first, heads, 2)
    gates = gates.transpose(1, 2, 0)
    more = padded - heads
    if more:
        gates = jnp.pad(gates, ((0, 0), (0, more), (0, 0)))
        extra_log_decay = jnp.pad(extra_log_decay, ((0, 0), (0, more), (0, 0)))
        head_decay_rate = jnp.pad(head_decay_rate, (0, more))
    gates = gates.reshape(2 * padded, width)
    table = max(128, 2 * padded)
    whole = pl.BlockSpec(memory_space=pltpu.VMEM)
    cut = pl.BlockSpec((width, head_dim), lambda t: (0, jnp.minimum(t, heads - 1)))
    block = (heads, seqs, head_dim, head_dim)
    return pl.pallas_call(
        functools.partial(kernel, parts),
        grid=(heads + parts - 1,),
        out_shape=(
            jax.ShapeDtypeStruct((seqs, heads, share, head_dim), bf16),
            jax.ShapeDtypeStruct((seqs, heads * head_dim), bf16),
        ),
        in_specs=[pl.BlockSpec(memory_space=pl.ANY), whole, cut, cut, cut]
        + [whole] * 4,
        out_specs=(whole, whole),
        scratch_shapes=[
            pltpu.VMEM((seqs * span + 128, width), bf16),
            pltpu.VMEM((table, seqs * span), f32),
            pltpu.VMEM((seqs * span, table), f32),
            pltpu.VMEM((2 * padded, 128), f32),
            pltpu.VMEM(block, f32),
            pltpu.VMEM(block, f32),
            pltpu.VMEM((heads, seqs, 8, head_dim), f32),
            pltpu.VMEM(block, f32),
            pltpu.VMEM(block, f32),
            pltpu.VMEM((heads, parts, seqs, share + 8, head_dim), f32),
            pltpu.VMEM((heads, seqs, share + 8, head_dim), f32),
            pltpu.SemaphoreType.DMA((seqs,)),
            pltpu.SemaphoreType.DMA((heads,)),
            pltpu.SemaphoreType.DMA((heads,)),
            pltpu.SemaphoreType.DMA((heads, parts)),
            pltpu.SemaphoreType.DMA((heads,)),
        ],
        compiler_params=pltpu.CompilerParams(
            collective_id=0,
            has_side_effects=True,
            dimension_semantics=("arbitrary",),
            vmem_limit_bytes=48 * 1024 * 1024,
        ),
    )(
        tokens,
        decoded_input,
        key_weight,
        value_weight,
        query_weight,
        gates,
        head_decay_rate.reshape(padded, 1),
        extra_log_decay,
        read_norm_gain.reshape(1, head_dim),
    )


def solution(mesh):
    in_specs = (
        P("grp", "sp", None),
        P("grp", None),
        P(None, "tp"),
        P(None, "tp"),
        P(None, "tp"),
        P(),
        P("tp"),
        P("grp", "tp", "sp"),
        P(),
    )
    out_specs = (P("grp", "tp", "sp", None), P("grp", "tp"))
    return jax.shard_map(
        functools.partial(per_device, mesh.shape["sp"]),
        mesh=mesh,
        in_specs=in_specs,
        out_specs=out_specs,
        check_vma=False,
    )
```
